512 devices in a mesh: tp: 32 (over z, x), dp: 16 (over y, core).
Axes of the slice: x: 4, y: 8, z: 8, core: 2. Of those that a mesh axis runs over, the one named last changes fastest.
Arguments:
- tokens: bfloat16 [256, 4096], P(None, 'dp'), may hold values from -6 to 6
- recurrent_state: float32 [2, 256, 262144], P(None, 'dp', 'tp'), may hold values from -24 to 24
- pre_gain: float32 [2, 4096], P(None, 'dp'), may hold values from 0.1 to 1.9
- w_query: bfloat16 [2, 4096, 2048], P(None, 'dp', 'tp'), may hold values from -0.09375 to 0.09375
- w_key: bfloat16 [2, 4096, 2048], P(None, 'dp', 'tp'), may hold values from -0.09375 to 0.09375
- w_value: bfloat16 [2, 4096, 4096], P(None, 'dp', 'tp'), may hold values from -0.09375 to 0.09375
- w_gate: bfloat16 [2, 4096, 4096], P(None, 'dp', 'tp'), may hold values from -0.09375 to 0.09375
- w_decay: bfloat16 [2, 4096, 2048], P(None, 'dp', 'tp'), may hold values from -1 to 1
- decay_bias: float32 [2, 2048], P(None, 'tp'), may hold values from -5 to 3
- head_gain: float32 [2, 128], replicated, may hold values from 0.1 to 1.9
- w_out: bfloat16 [2, 4096, 4096], P(None, 'tp', 'dp'), may hold values from -0.09375 to 0.09375
- post_gain: float32 [2, 4096], P(None, 'dp'), may hold values from 0.1 to 1.9
Outputs:
- hidden_out: bfloat16 [256, 4096], P(None, 'dp')
- state_out: float32 [2, 256, 262144], P(None, 'dp', 'tp')
The draws below stay inside these ranges and needn't reach their ends.
All inputs are finite; a program needn't handle non-finite values.
Results may differ from the reference program's by a relative error of at most 0.015.
Values may be sent and summed in bfloat16 or wider, within the bound.
A program may use at most 64 MiB of HBM per device.

```python
import jax
import jax.numpy as jnp
from jax import lax

D = 4096
HEADS = 32
KEY = 64
VAL = 128
QK = 2048
VW = 4096
SEQS = 256


def draw_recurrent_state(key, part):
    shape = (2, SEQS, VW * KEY)
    column = jnp.arange(VW * KEY, dtype=jnp.int32) // KEY
    within = (column % VAL).astype(jnp.float32) / (VAL - 1)
    ratio = 6.0
    noise = jnp.clip(jax.random.normal(key, shape, jnp.float32), -4.0, 4.0)
    scale = 0.5 * jnp.exp(jnp.log(ratio) * within)
    return (noise * scale[None, None, :]).astype(jnp.float32)


def levels(key, shape, split, smallest, high):
    level = 1.0
    for axis_at, blocks in split:
        heights = jax.random.uniform(jax.random.fold_in(jax.random.fold_in(key, 6), axis_at), (blocks,), jnp.float32, smallest / len(split), high / len(split))
        level = level * jnp.repeat(jnp.exp(heights), shape[axis_at] // blocks).reshape((-1,) + (1,) * (len(shape) - 1 - axis_at))
    return level


def scatter_about(key, shape, scale, reach, cuts=(), kind=jnp.bfloat16):
    values = jax.random.normal(key, shape, jnp.float32) * scale
    if len(cuts) > 0:
        values = levels(key, shape, cuts, -0.22, 0.18) * values
    return jnp.clip(values, min=-reach, max=reach).astype(kind)


def setup_inputs(seed: int = 0) -> dict:
    key_of = jax.random.split(jax.random.key(seed), 13)
    return {
        "tokens": scatter_about(key_of[0], (SEQS, D), 1.0, 6.0, ((1, 16),)),
        "recurrent_state": draw_recurrent_state(jax.random.fold_in(key_of[12], 71), 0),
        "pre_gain": jnp.clip(1.0 + 0.18 * jax.random.normal(key_of[2], (2, D), jnp.float32), 0.1, 1.9),
        "w_query": scatter_about(key_of[3], (2, D, QK), D ** -0.5, 0.09375, ((1, 16), (2, 32))),
        "w_key": scatter_about(key_of[4], (2, D, QK), D ** -0.5, 0.09375, ((1, 16), (2, 32))),
        "w_value": scatter_about(key_of[5], (2, D, VW), D ** -0.5, 0.09375, ((1, 16), (2, 32))),
        "w_gate": scatter_about(key_of[6], (2, D, VW), D ** -0.5, 0.09375, ((1, 16), (2, 32))),
        "w_decay": scatter_about(key_of[7], (2, D, QK), 0.0625, 1.0, ((1, 16), (2, 32))),
        "decay_bias": jnp.clip(-5.0 + 8.0 * jax.random.uniform(key_of[8], (2, QK), jnp.float32) ** levels(key_of[8], (2, QK), ((1, 32),), -0.2, 0.2), -5.0, 3.0),
        "head_gain": jnp.clip(1.0 + 0.18 * jax.random.normal(key_of[9], (2, VAL), jnp.float32), 0.1, 1.9),
        "w_out": scatter_about(key_of[10], (2, VW, D), VW ** -0.5, 0.09375, ((1, 32), (2, 16))),
        "post_gain": jnp.clip(1.0 + 0.18 * jax.random.normal(key_of[11], (2, D), jnp.float32), 0.1, 1.9),
    }


epsilon = 1e-06

def reference(tokens, recurrent_state, pre_gain, w_query, w_key, w_value, w_gate, w_decay, decay_bias, head_gain, w_out, post_gain):
    residual = tokens
    new_states = []
    for section_index in range(2):
        wide_float = residual.astype(jnp.float32)
        row_scale = lax.rsqrt(lax.optimization_barrier(jnp.mean(wide_float * wide_float, axis=1, keepdims=True)) + epsilon)
        normed = (wide_float * pre_gain[section_index]).astype(jnp.bfloat16)

        def project_role(weights):
            return jnp.dot(normed, weights[section_index], preferred_element_type=jnp.float32) * row_scale
        query = lax.optimization_barrier(project_role(w_query).astype(jnp.bfloat16)).astype(jnp.float32)
        key_vec = lax.optimization_barrier(project_role(w_key).astype(jnp.bfloat16)).astype(jnp.float32)
        values_own = project_role(w_value)
        gate_pre = project_role(w_gate)
        log_decay = jax.nn.log_sigmoid(project_role(w_decay) + decay_bias[section_index]) / 16.0
        seq_count = residual.shape[0]
        query = query.reshape(seq_count, HEADS, 1, KEY)
        key_vec = key_vec.reshape(seq_count, HEADS, 1, KEY)
        decay_rate = jnp.exp(log_decay).reshape(seq_count, HEADS, 1, KEY)
        old_state = recurrent_state[section_index].reshape(seq_count, HEADS, VAL, KEY)
        new_state = decay_rate * old_state + key_vec * values_own.reshape(seq_count, HEADS, VAL, 1)
        readout = lax.optimization_barrier(jnp.sum(query * new_state, axis=3)) * KEY ** (-0.5)
        head_mean = lax.optimization_barrier(jnp.mean(readout * readout, axis=-1, keepdims=True))
        mixed = readout * lax.rsqrt(head_mean + epsilon) * head_gain[section_index] * jax.nn.silu(gate_pre.reshape(seq_count, HEADS, VAL))
        mixed = mixed.reshape(seq_count, HEADS * VAL).astype(jnp.bfloat16)
        out_rows = jnp.dot(mixed, w_out[section_index], preferred_element_type=jnp.float32)
        out_scale = lax.rsqrt(lax.optimization_barrier(jnp.mean(out_rows * out_rows, axis=1, keepdims=True)) + epsilon)
        residual = (wide_float + out_rows * out_scale * post_gain[section_index]).astype(jnp.bfloat16)
        new_states.append(new_state.reshape(seq_count, HEADS * VAL * KEY))
    return (residual, jnp.stack(new_states))
```

```python
import jax
import jax.numpy as jnp
from jax import lax
from jax.experimental import pallas as pl
from jax.experimental.pallas import tpu as pltpu
from jax.sharding import PartitionSpec as P

MESH = pl.DeviceIdType.MESH
D = 4096
KEY = 64
VAL = 128
NX, NY, NZ = 4, 8, 8
ROWS = 16
EPS = 1e-6
F32 = jnp.float32
BF16 = jnp.bfloat16


def ring(step, size):
    return min(step, size - step)


Y_STEPS = sorted(range(1, NY), key=lambda a: -ring(a, NY))
XZ_STEPS = sorted(
    ((a, b) for a in range(NX) for b in range(NZ) if a or b),
    key=lambda s: -ring(s[0], NX) - ring(s[1], NZ),
)


def lanes(shape):
    return lax.broadcasted_iota(jnp.int32, shape, 1)


def halves(value):
    high = value.astype(BF16)
    return high.astype(F32), (value - high.astype(F32))


def with_columns(tile, columns):
    at = lanes(tile.shape)
    for place, column in columns:
        tile = jnp.where(at == place, column, tile)
    return tile


def split_columns(stats):
    columns = []
    for i, stat in enumerate(stats):
        high, low = halves(stat)
        columns += [(KEY + 2 * i, high), (KEY + 2 * i + 1, low)]
    return columns


def stat_of(tile, i):
    return tile[:, KEY + 2 * i : KEY + 2 * i + 1] + tile[:, KEY + 2 * i + 1 : KEY + 2 * i + 2]


def kernel(
    tok_hbm, state_hbm, pre_hbm, wq_hbm, wk_hbm, wv_hbm, wg_hbm, wd_hbm, bias_hbm, hgain_hbm, wo_hbm, post_hbm,
    hid_hbm, snew_hbm,
    tok, x0, state, pre, post, bias, hgain, wq, wk, wd, w0, w1, wo,
    psend, precv, asend0, arecv0, asend1, arecv1, p1send, p1recv,
    b0, b1, csend0, csend1, crecv0, crecv1, dsend0, dsend1, d0, d1,
    ssend, srecv, hsend, hout,
    load, xsend, xrecv, phase_send, phase_recv, ready, outs,
):
    tp, dp = lax.axis_index("tp"), lax.axis_index("dp")
    z, x = tp // NX, lax.rem(tp, NX)
    y, c = dp // 2, lax.rem(dp, 2)
    other = 1 - c

    def place(dx=0, dy=0, dz=0):
        return {
            "tp": lax.rem(z + dz, NZ) * NX + lax.rem(x + dx, NX),
            "dp": lax.rem(y + dy, NY) * 2 + c,
        }

    partner = {"tp": tp, "dp": y * 2 + other}

    def fetch(source, target, i):
        copy = pltpu.make_async_copy(source, target, load.at[i])
        copy.start()
        return copy

    for a in range(NY):
        pltpu.make_async_copy(tok_hbm.at[lax.rem(y + NY - a, NY)], tok.at[:, a], load.at[0]).start()
    first = [
        fetch(pre_hbm, pre.at[c], 1),
        fetch(wq_hbm.at[0], wq.at[0], 2),
        fetch(wk_hbm.at[0], wk.at[0], 3),
        fetch(wd_hbm.at[0], wd.at[0], 4),
        fetch(wv_hbm.at[0], w0.at[:, pl.ds(0, 128)], 5),
        fetch(wg_hbm.at[0], w0.at[:, pl.ds(128, 128)], 6),
    ]
    second = [
        fetch(post_hbm, post.at[c], 7),
        fetch(wq_hbm.at[1], wq.at[1], 8),
        fetch(wk_hbm.at[1], wk.at[1], 9),
        fetch(wd_hbm.at[1], wd.at[1], 10),
        fetch(wv_hbm.at[1], w1.at[c, :, pl.ds(0, 128)], 11),
        fetch(wg_hbm.at[1], w1.at[c, :, pl.ds(128, 128)], 12),
        fetch(wo_hbm, wo.at[c], 13),
        fetch(bias_hbm, bias, 14),
        fetch(hgain_hbm, hgain, 15),
    ]
    third = [fetch(state_hbm, state, 16)]

    barrier = pltpu.get_barrier_semaphore()
    pl.semaphore_signal(barrier, inc=1, device_id=partner, device_id_type=MESH)
    for a in Y_STEPS:
        pl.semaphore_signal(barrier, inc=1, device_id=place(dy=a), device_id_type=MESH)
    for a in range(1, NZ):
        pl.semaphore_signal(barrier, inc=1, device_id=place(dz=a), device_id_type=MESH)
    for a in range(1, NX):
        pl.semaphore_signal(barrier, inc=1, device_id=place(dx=a), device_id_type=MESH)

    def join_weights(section, target):
        q, k, decay = wq[section], wk[section], wd[section]
        target[:, 256:384] = jnp.concatenate([q, k], axis=1)
        target[:, 384:512] = jnp.concatenate([decay, jnp.zeros_like(decay)], axis=1)

    pltpu.make_async_copy(tok, tok, load.at[0]).wait()
    for copy in first:
        copy.wait()
    join_weights(0, w0)

    def project_first(half):
        wide = tok[half].reshape(NY * ROWS, 256).astype(F32)
        normed = (wide * pre[c, 0:1, :]).astype(BF16)
        out = jnp.dot(normed, w0[...], preferred_element_type=F32)
        squares = jnp.sum(wide * wide, axis=1, keepdims=True)
        return jnp.concatenate(
            [out[:, :384], with_columns(out[:, 384:], split_columns([squares]))], axis=1
        )

    psend[...] = project_first(other).astype(BF16)
    own = project_first(c)
    pl.semaphore_wait(barrier, 1 + (NY - 1) + (NZ - 1) + (NX - 1))

    def send(source, target, device, i, sems):
        copy = pltpu.make_async_remote_copy(
            src_ref=source, dst_ref=target, send_sem=sems[0].at[i], recv_sem=sems[1].at[i],
            device_id=device, device_id_type=MESH,
        )
        copy.start()
        return copy

    swap = (xsend, xrecv)
    partial = send(psend, precv, partner, 0, swap)
    for a in range(1, NZ):
        pl.semaphore_signal(ready, inc=1, device_id=place(dz=a), device_id_type=MESH)

    step = (phase_send, phase_recv)

    def send_along_y(source, target, i):
        for a in Y_STEPS:
            send(source.at[a], target.at[a - 1], place(dy=NY - a), i, step)

    def arrived(ref, i):
        pltpu.make_async_copy(ref, ref, phase_recv.at[i]).wait()

    def sent(ref, i):
        pltpu.make_async_copy(ref, ref, phase_send.at[i]).wait()

    partial.wait_recv()
    own = own + precv[...].astype(F32)
    asend0[...] = own.astype(BF16).reshape(NY, ROWS, 512)
    send_along_y(asend0, arecv0, 0)
    own0 = own[:ROWS]

    for copy in second:
        copy.wait()
    join_weights(1, w1.at[c])
    exchanged = [
        send(tok.at[other], x0.at[c], partner, 1, swap),
        send(pre.at[c], pre.at[c], partner, 2, swap),
        send(post.at[c], post.at[c], partner, 3, swap),
        send(wo.at[c], wo.at[c], partner, 4, swap),
        send(w1.at[c], w1.at[c], partner, 5, swap),
    ]
    x0[c] = tok[c]
    for copy in third:
        copy.wait()

    def summed(own_rows, ref):
        total = own_rows
        for i in range(ref.shape[0]):
            total = total + ref[i].astype(F32)
        return total

    lane = lanes((ROWS, 128))
    half_sum = (
        lax.broadcasted_iota(jnp.int32, (128, 128), 0) // KEY == lax.rem(lanes((128, 128)), 2)
    ).astype(F32).astype(BF16)

    def attend(section, proj):
        values, gate = proj[:, 0:128], proj[:, 128:256]
        query = proj[:, 256:320].astype(BF16).astype(F32)
        key = proj[:, 320:384].astype(BF16).astype(F32)
        pre_decay = proj[:, 384:448] + bias[section : section + 1, :]
        log_sigmoid = jnp.minimum(pre_decay, 0.0) - jnp.log(1.0 + jnp.exp(-jnp.abs(pre_decay)))
        decay = jnp.exp(log_sigmoid / 16.0)
        faded = query * decay
        faded2 = jnp.concatenate([faded, faded], axis=1)
        terms = jnp.concatenate(
            [state[section, :, 128 * j : 128 * (j + 1)] * faded2 for j in range(KEY)], axis=0
        )
        high = terms.astype(BF16)
        low = (terms - high.astype(F32)).astype(BF16)
        sums = jnp.dot(high, half_sum, preferred_element_type=F32) + jnp.dot(
            low, half_sum, preferred_element_type=F32
        )
        old_part = jnp.zeros((ROWS, 128), F32)
        for j in range(KEY):
            old_part = jnp.where(lane // 2 == j, sums[ROWS * j : ROWS * (j + 1)], old_part)
        readout = (old_part + values * jnp.sum(query * key, axis=1, keepdims=True)) * KEY**-0.5
        mean = jnp.mean(readout * readout, axis=1, keepdims=True)
        gated = gate / (1.0 + jnp.exp(-gate))
        mixed = readout * lax.rsqrt(mean + EPS) * hgain[section : section + 1, :] * gated
        return mixed.astype(BF16), (values, key, decay)

    def update_state(section, parts):
        values, key, decay = parts
        decay2 = jnp.concatenate([decay, decay], axis=1)
        key2 = jnp.concatenate([key, key], axis=1)
        for j in range(KEY):
            value = jnp.where(lane < KEY, values[:, 2 * j : 2 * j + 1], values[:, 2 * j + 1 : 2 * j + 2])
            tile = pl.ds(128 * j, 128)
            state[section, :, tile] = decay2 * state[section, :, tile] + key2 * value
        copy = pltpu.make_async_copy(state.at[section], snew_hbm.at[section], outs.at[section])
        copy.start()
        return copy

    def send_mixed(mixed, b, i):
        b[0] = mixed
        for a in Y_STEPS:
            send(b.at[0], b.at[a], place(dy=a), i, step)

    def project_out(section, b, csend):
        gathered = b[...].reshape(NY * ROWS, 128)
        for half in range(2):
            out = jnp.dot(gathered, wo[half, section], preferred_element_type=F32).astype(BF16)
            for zz in range(NZ):
                for part in range(2):
                    csend[zz * NX + half * 2 + part] = out[ROWS * zz : ROWS * (zz + 1), 128 * part : 128 * (part + 1)]

    def send_sums(csend, crecv, i):
        for n, (a, b) in enumerate(XZ_STEPS):
            block = lax.rem(z + b, NZ) * NX + lax.rem(x + a, NX)
            send(csend.at[block], crecv.at[n], place(dx=a, dz=b), i, step)

    def send_rows(rows, dsend, d, i):
        mine = x * NZ + z
        dsend[...] = rows
        d[mine] = rows
        for a, b in XZ_STEPS:
            send(dsend, d.at[mine], place(dx=a, dz=b), i, step)

    arrived(arecv0, 0)
    total0 = summed(own0, arecv0)
    squares0 = stat_of(total0[:, 384:], 0)
    scale0 = lax.rsqrt(squares0 / D + EPS)
    mixed, parts = attend(0, total0[:, :448] * scale0)
    send_mixed(mixed, b0, 1)
    wrote = [update_state(0, parts)]

    for copy in exchanged:
        copy.wait_recv()

    def project_tokens():
        out = None
        for half in range(2):
            wide = x0[half].reshape(NY * ROWS, 256).astype(F32)
            normed = (wide * pre[half, 1:2, :]).astype(BF16)
            term = jnp.dot(normed, w1[half], preferred_element_type=F32)
            out = term if out is None else out + term
        return out

    from_tokens = project_tokens()
    p1send[...] = from_tokens.astype(BF16).reshape(NY, ROWS, 512)
    own_tokens = from_tokens[:ROWS]

    arrived(b0.at[pl.ds(1, NY - 1)], 1)
    project_out(0, b0, csend0)
    pl.semaphore_wait(ready, NZ - 1)
    send_sums(csend0, crecv0, 2)
    send_along_y(p1send, p1recv, 4)
    arrived(crecv0, 2)
    send_rows(summed(csend0[z * NX + x].astype(F32), crecv0).astype(BF16), dsend0, d0, 3)
    arrived(p1recv, 4)
    total_tokens = summed(own_tokens, p1recv)

    arrived(d0.at[pl.ds(0, NX * NZ - 1)], 3)
    out = jnp.zeros((NY * ROWS, 512), F32)
    squares_out = cross = squares_step = jnp.zeros((NY * ROWS, 1), F32)
    for half in range(2):
        rows = [
            d0[pl.ds(NZ * (2 * half + part), NZ)].reshape(NZ * ROWS, 128).astype(F32) for part in range(2)
        ]
        rows = jnp.concatenate(rows, axis=1)
        moved = rows * post[half, 0:1, :]
        wide = x0[half].reshape(NY * ROWS, 256).astype(F32)
        squares_out += jnp.sum(rows * rows, axis=1, keepdims=True)
        cross += jnp.sum(wide * moved, axis=1, keepdims=True)
        squares_step += jnp.sum(moved * moved, axis=1, keepdims=True)
        normed = (moved * pre[half, 1:2, :]).astype(BF16)
        out += jnp.dot(normed, w1[half], preferred_element_type=F32)
    own = jnp.concatenate(
        [out[:, :384], with_columns(out[:, 384:], split_columns([squares_out, cross, squares_step]))], axis=1
    )
    asend1[...] = own.astype(BF16).reshape(NY, ROWS, 512)
    send_along_y(asend1, arecv1, 5)
    own1 = own[:ROWS]
    arrived(arecv1, 5)
    total1 = summed(own1, arecv1)
    tail = total1[:, 384:]
    step_scale = lax.rsqrt(stat_of(tail, 0) / D + EPS)
    squares1 = squares0 + step_scale * (2.0 * stat_of(tail, 1) + step_scale * stat_of(tail, 2))
    scale1 = lax.rsqrt(jnp.maximum(squares1, 0.0) / D + EPS)
    mixed, parts = attend(1, (total_tokens[:, :448] + step_scale * total1[:, :448]) * scale1)
    send_mixed(mixed, b1, 6)
    wrote.append(update_state(1, parts))
    arrived(b1.at[pl.ds(1, NY - 1)], 6)
    project_out(1, b1, csend1)
    send_sums(csend1, crecv1, 7)
    arrived(crecv1, 7)
    send_rows(summed(csend1[z * NX + x].astype(F32), crecv1).astype(BF16), dsend1, d1, 8)
    arrived(d1.at[pl.ds(0, NX * NZ - 1)], 8)

    squares_last = jnp.zeros((NY * ROWS, 1), F32)
    for part in range(NX):
        rows = d1[pl.ds(NZ * part, NZ)].reshape(NZ * ROWS, 128).astype(F32)
        squares_last += jnp.sum(rows * rows, axis=1, keepdims=True)
    tile = jnp.zeros((ROWS, 128), F32)
    for a in range(NY):
        at = lax.rem(y + NY - a, NY)
        tile = jnp.where(lane == at, squares_last[ROWS * a : ROWS * (a + 1)], tile)
        tile = jnp.where(lane == NY + at, squares_out[ROWS * a : ROWS * (a + 1)], tile)
    ssend[...] = tile
    for a in Y_STEPS:
        send(ssend, srecv.at[a - 1], place(dy=a), 9, step)
    arrived(srecv, 9)
    scales = lax.rsqrt(summed(tile, srecv) / D + EPS)

    def finish(half, target):
        for a in range(NY):
            at = lax.rem(y + NY - a, NY)
            last = jnp.sum(jnp.where(lane == at, scales, 0.0), axis=1, keepdims=True)
            before = jnp.sum(jnp.where(lane == NY + at, scales, 0.0), axis=1, keepdims=True)
            for part in range(2):
                cols = pl.ds(128 * part, 128)
                slot = NZ * (2 * half + part) + a
                gain = post[half, :, cols]
                value = (
                    x0[half, a, :, cols].astype(F32)
                    + d0[slot].astype(F32) * before * gain[0:1]
                    + d1[slot].astype(F32) * last * gain[1:2]
                )
                target(at)[:, cols] = value.astype(BF16)

    finish(other, lambda at: hsend.at[at])
    result = send(hsend, hout.at[:, c], partner, 6, swap)
    finish(c, lambda at: hout.at[at, c])
    result.wait_recv()
    copy = pltpu.make_async_copy(hout, hid_hbm, outs.at[2])
    copy.start()
    wrote.append(copy)

    partial.wait_send()
    result.wait_send()
    for copy in exchanged:
        copy.wait_send()
    for ref, i in (
        (arecv0, 0), (arecv1, 5), (p1recv, 4), (b0.at[pl.ds(1, NY - 1)], 1), (b1.at[pl.ds(1, NY - 1)], 6),
        (crecv0, 2), (crecv1, 7), (d0.at[pl.ds(0, NX * NZ - 1)], 3), (d1.at[pl.ds(0, NX * NZ - 1)], 8), (srecv, 9),
    ):
        sent(ref, i)
    for copy in wrote:
        copy.wait()


def local(tokens, recurrent_state, pre_gain, w_query, w_key, w_value, w_gate, w_decay, decay_bias, head_gain, w_out, post_gain):
    vmem = pltpu.VMEM
    dma = pltpu.SemaphoreType.DMA
    blocks = NX * NZ
    hidden, state = pl.pallas_call(
        kernel,
        out_shape=(
            jax.ShapeDtypeStruct((NY, 2, ROWS, 256), BF16),
            jax.ShapeDtypeStruct((2, ROWS, VAL * KEY), F32),
        ),
        in_specs=[pl.BlockSpec(memory_space=pl.ANY)] * 12,
        out_specs=[pl.BlockSpec(memory_space=pl.ANY)] * 2,
        scratch_shapes=[
            vmem((2, NY, ROWS, 256), BF16),
            vmem((2, NY, ROWS, 256), BF16),
            vmem((2, ROWS, VAL * KEY), F32),
            vmem((2, 2, 256), F32),
            vmem((2, 2, 256), F32),
            vmem((2, KEY), F32),
            vmem((2, VAL), F32),
            vmem((2, 256, KEY), BF16),
            vmem((2, 256, KEY), BF16),
            vmem((2, 256, KEY), BF16),
            vmem((256, 512), BF16),
            vmem((2, 256, 512), BF16),
            vmem((2, 2, 128, 256), BF16),
            vmem((NY * ROWS, 512), BF16),
            vmem((NY * ROWS, 512), BF16),
            vmem((NY, ROWS, 512), BF16),
            vmem((NY - 1, ROWS, 512), BF16),
            vmem((NY, ROWS, 512), BF16),
            vmem((NY - 1, ROWS, 512), BF16),
            vmem((NY, ROWS, 512), BF16),
            vmem((NY - 1, ROWS, 512), BF16),
            vmem((NY, ROWS, 128), BF16),
            vmem((NY, ROWS, 128), BF16),
            vmem((blocks, ROWS, 128), BF16),
            vmem((blocks, ROWS, 128), BF16),
            vmem((blocks - 1, ROWS, 128), BF16),
            vmem((blocks - 1, ROWS, 128), BF16),
            vmem((ROWS, 128), BF16),
            vmem((ROWS, 128), BF16),
            vmem((blocks, ROWS, 128), BF16),
            vmem((blocks, ROWS, 128), BF16),
            vmem((ROWS, 128), F32),
            vmem((NY - 1, ROWS, 128), F32),
            vmem((NY, ROWS, 256), BF16),
            vmem((NY, 2, ROWS, 256), BF16),
            dma((17,)),
            dma((7,)),
            dma((7,)),
            dma((10,)),
            dma((10,)),
            pltpu.SemaphoreType.REGULAR,
            dma((3,)),
        ],
        compiler_params=pltpu.CompilerParams(
            collective_id=0, has_side_effects=True, vmem_limit_bytes=32 * 1024 * 1024
        ),
    )(
        tokens.reshape(NY, 2, ROWS, 256), recurrent_state, pre_gain, w_query, w_key, w_value, w_gate, w_decay,
        decay_bias, head_gain, w_out, post_gain,
    )
    return hidden.reshape(NY * 2 * ROWS, 256), state


def solution(mesh):
    in_specs = (
        P(None, "dp"), P(None, "dp", "tp"), P(None, "dp"), P(None, "dp", "tp"), P(None, "dp", "tp"),
        P(None, "dp", "tp"), P(None, "dp", "tp"), P(None, "dp", "tp"), P(None, "tp"), P(), P(None, "tp", "dp"),
        P(None, "dp"),
    )
    out_specs = (P(None, "dp"), P(None, "dp", "tp"))
    return jax.shard_map(local, mesh=mesh, in_specs=in_specs, out_specs=out_specs, check_vma=False)
```

```python
import jax
import jax.numpy as jnp
from jax import lax
from jax.experimental import pallas as pl
from jax.experimental.pallas import tpu as pltpu
from jax.sharding import PartitionSpec as P

MESH = pl.DeviceIdType.MESH
D = 4096
KEY = 64
VAL = 128
NX, NY, NZ = 4, 8, 8
ROWS = 16
EPS = 1e-6
F32 = jnp.float32
BF16 = jnp.bfloat16


def ring(step, size):
    return min(step, size - step)


Y_STEPS = sorted(range(1, NY), key=lambda a: -ring(a, NY))
XZ_STEPS = sorted(
    ((a, b) for a in range(NX) for b in range(NZ) if a or b),
    key=lambda s: -ring(s[0], NX) - ring(s[1], NZ),
)


def lanes(shape):
    return lax.broadcasted_iota(jnp.int32, shape, 1)


def halves(value):
    high = value.astype(BF16)
    return high.astype(F32), (value - high.astype(F32))


def with_columns(tile, columns):
    at = lanes(tile.shape)
    for place, column in columns:
        tile = jnp.where(at == place, column, tile)
    return tile


def split_columns(stats):
    columns = []
    for i, stat in enumerate(stats):
        high, low = halves(stat)
        columns += [(KEY + 2 * i, high), (KEY + 2 * i + 1, low)]
    return columns


def stat_of(tile, i):
    return tile[:, KEY + 2 * i : KEY + 2 * i + 1] + tile[:, KEY + 2 * i + 1 : KEY + 2 * i + 2]


def kernel(
    tok_hbm, state_hbm, pre_hbm, wq_hbm, wk_hbm, wv_hbm, wg_hbm, wd_hbm, bias_hbm, hgain_hbm, wo_hbm, post_hbm,
    hid_hbm, snew_hbm,
    tok, x0, state, pre, post, bias, hgain, w0, w1, wo0, wo1,
    psend, precv, asend0, arecv0, asend1, arecv1, p1send, p1recv,
    b0, csend0, csend1, crecv0, crecv1, dsend0, dsend1, d0, d1, dpart,
    ssend, srecv, base, esend, erecv, hout,
    load, xsend, xrecv, phase_send, phase_recv, ready, outs,
):
    tp, dp = lax.axis_index("tp"), lax.axis_index("dp")
    z, x = tp // NX, lax.rem(tp, NX)
    y, c = dp // 2, lax.rem(dp, 2)
    other = 1 - c

    def place(dx=0, dy=0, dz=0):
        return {
            "tp": lax.rem(z + dz, NZ) * NX + lax.rem(x + dx, NX),
            "dp": lax.rem(y + dy, NY) * 2 + c,
        }

    partner = {"tp": tp, "dp": y * 2 + other}

    def fetch(source, target, i):
        copy = pltpu.make_async_copy(source, target, load.at[i])
        copy.start()
        return copy

    def fetch_weights(section, target, i):
        return [
            fetch(wv_hbm.at[section], target.at[0, :, pl.ds(0, 128)], i),
            fetch(wg_hbm.at[section], target.at[0, :, pl.ds(128, 128)], i + 1),
            fetch(wq_hbm.at[section], target.at[1, pl.ds(0, KEY)], i + 2),
            fetch(wk_hbm.at[section], target.at[1, pl.ds(KEY, KEY)], i + 3),
            fetch(wd_hbm.at[section], target.at[1, pl.ds(2 * KEY, KEY)], i + 4),
        ]

    def project(rows, weights):
        return jnp.concatenate(
            [
                jnp.dot(rows, weights[0], preferred_element_type=F32),
                lax.dot_general(rows, weights[1], (((1,), (1,)), ((), ())), preferred_element_type=F32),
            ],
            axis=1,
        )

    for a in range(NY):
        pltpu.make_async_copy(tok_hbm.at[lax.rem(y + NY - a, NY)], tok.at[:, a], load.at[0]).start()
    first = [
        fetch(pre_hbm, pre.at[c], 1),
        *fetch_weights(0, w0, 2),
    ]
    second = [
        fetch(post_hbm, post.at[c], 7),
        *fetch_weights(1, w1.at[c], 8),
        fetch(wo_hbm.at[0], wo0.at[c], 13),
        fetch(wo_hbm.at[1], wo1.at[0, c], 17),
        fetch(bias_hbm, bias, 14),
        fetch(hgain_hbm, hgain, 15),
    ]
    third = [fetch(state_hbm, state, 16)]

    barrier = pltpu.get_barrier_semaphore()
    pl.semaphore_signal(barrier, inc=1, device_id=partner, device_id_type=MESH)
    for a in Y_STEPS:
        pl.semaphore_signal(barrier, inc=1, device_id=place(dy=a), device_id_type=MESH)
    for a in range(1, NZ):
        pl.semaphore_signal(barrier, inc=1, device_id=place(dz=a), device_id_type=MESH)
    for a in range(1, NX):
        pl.semaphore_signal(barrier, inc=1, device_id=place(dx=a), device_id_type=MESH)

    pltpu.make_async_copy(tok, tok, load.at[0]).wait()
    for copy in first:
        copy.wait()
    w0[1, 3 * KEY :] = jnp.zeros((KEY, 256), BF16)

    def project_first(half):
        wide = tok[half].reshape(NY * ROWS, 256).astype(F32)
        normed = (wide * pre[c, 0:1, :]).astype(BF16)
        out = project(normed, w0)
        squares = jnp.sum(wide * wide, axis=1, keepdims=True)
        return jnp.concatenate(
            [out[:, :384], with_columns(out[:, 384:], split_columns([squares]))], axis=1
        )

    psend[...] = project_first(other).astype(BF16)
    own = project_first(c)
    pl.semaphore_wait(barrier, 1 + (NY - 1) + (NZ - 1) + (NX - 1))

    def send(source, target, device, i, sems):
        copy = pltpu.make_async_remote_copy(
            src_ref=source, dst_ref=target, send_sem=sems[0].at[i], recv_sem=sems[1].at[i],
            device_id=device, device_id_type=MESH,
        )
        copy.start()
        return copy

    swap = (xsend, xrecv)
    partial = send(psend, precv, partner, 0, swap)
    for a in range(1, NZ):
        pl.semaphore_signal(ready, inc=1, device_id=place(dz=a), device_id_type=MESH)

    step = (phase_send, phase_recv)

    def send_along_y(source, target, i):
        for a in Y_STEPS:
            send(source.at[a], target.at[a - 1], place(dy=NY - a), i, step)

    def arrived(ref, i):
        pltpu.make_async_copy(ref, ref, phase_recv.at[i]).wait()

    def sent(ref, i):
        pltpu.make_async_copy(ref, ref, phase_send.at[i]).wait()

    partial.wait_recv()
    own = own + precv[...].astype(F32)
    asend0[...] = own.astype(BF16).reshape(NY, ROWS, 512)
    send_along_y(asend0, arecv0, 0)
    own0 = own[:ROWS]

    for copy in second:
        copy.wait()
    w1[c, 1, 3 * KEY :] = jnp.zeros((KEY, 256), BF16)
    exchanged = [
        send(tok.at[other], x0.at[c], partner, 1, swap),
        send(pre.at[c], pre.at[c], partner, 2, swap),
        send(post.at[c], post.at[c], partner, 3, swap),
        send(wo0.at[c], wo0.at[c], partner, 4, swap),
        send(wo1.at[0, c], wo1.at[0, c], partner, 6, swap),
        send(w1.at[c], w1.at[c], partner, 5, swap),
    ]
    x0[c] = tok[c]
    for copy in third:
        copy.wait()

    def summed(own_rows, ref):
        total = own_rows
        for i in range(ref.shape[0]):
            total = total + ref[i].astype(F32)
        return total

    lane = lanes((ROWS, 128))
    half_sum = (
        lax.broadcasted_iota(jnp.int32, (128, 128), 0) // KEY == lax.rem(lanes((128, 128)), 2)
    ).astype(F32).astype(BF16)

    def attend(section, proj):
        values, gate = proj[:, 0:128], proj[:, 128:256]
        query = proj[:, 256:320].astype(BF16).astype(F32)
        key = proj[:, 320:384].astype(BF16).astype(F32)
        pre_decay = proj[:, 384:448] + bias[section : section + 1, :]
        log_sigmoid = jnp.minimum(pre_decay, 0.0) - jnp.log(1.0 + jnp.exp(-jnp.abs(pre_decay)))
        decay = jnp.exp(log_sigmoid / 16.0)
        faded = query * decay
        faded2 = jnp.concatenate([faded, faded], axis=1)
        terms = jnp.concatenate(
            [state[section, :, 128 * j : 128 * (j + 1)] * faded2 for j in range(KEY)], axis=0
        )
        high = terms.astype(BF16)
        low = (terms - high.astype(F32)).astype(BF16)
        sums = jnp.dot(high, half_sum, preferred_element_type=F32) + jnp.dot(
            low, half_sum, preferred_element_type=F32
        )
        old_part = jnp.zeros((ROWS, 128), F32)
        for j in range(KEY):
            old_part = jnp.where(lane // 2 == j, sums[ROWS * j : ROWS * (j + 1)], old_part)
        readout = (old_part + values * jnp.sum(query * key, axis=1, keepdims=True)) * KEY**-0.5
        mean = jnp.mean(readout * readout, axis=1, keepdims=True)
        gated = gate / (1.0 + jnp.exp(-gate))
        mixed = readout * lax.rsqrt(mean + EPS) * hgain[section : section + 1, :] * gated
        return mixed.astype(BF16), (values, key, decay)

    def update_state(section, parts):
        values, key, decay = parts
        decay2 = jnp.concatenate([decay, decay], axis=1)
        key2 = jnp.concatenate([key, key], axis=1)
        for j in range(KEY):
            value = jnp.where(lane < KEY, values[:, 2 * j : 2 * j + 1], values[:, 2 * j + 1 : 2 * j + 2])
            tile = pl.ds(128 * j, 128)
            state[section, :, tile] = decay2 * state[section, :, tile] + key2 * value
        copy = pltpu.make_async_copy(state.at[section], snew_hbm.at[section], outs.at[section])
        copy.start()
        return copy

    def send_mixed(mixed, b, i):
        b[0] = mixed
        for a in Y_STEPS:
            send(b.at[0], b.at[a], place(dy=a), i, step)

    def project_out_here(b, csend):
        gathered = b[...].reshape(NY * ROWS, 128)
        for half in range(2):
            out = jnp.dot(gathered, wo0[half], preferred_element_type=F32).astype(BF16)
            for zz in range(NZ):
                for part in range(2):
                    csend[zz * NX + half * 2 + part] = out[ROWS * zz : ROWS * (zz + 1), 128 * part : 128 * (part + 1)]

    def project_out_all(mixed, csend):
        for back in range(NY):
            for half in range(2):
                out = jnp.dot(mixed, wo1[back, half], preferred_element_type=F32).astype(BF16)
                for part in range(2):
                    csend[back * NX + half * 2 + part] = out[:, 128 * part : 128 * (part + 1)]

    def send_sums(csend, crecv, i):
        for n, (a, b) in enumerate(XZ_STEPS):
            block = lax.rem(z + b, NZ) * NX + lax.rem(x + a, NX)
            send(csend.at[block], crecv.at[n], place(dx=a, dz=b), i, step)

    def send_rows(rows, dsend, d, i):
        mine = x * NZ + z
        dsend[...] = rows
        d[mine] = rows
        for a, b in XZ_STEPS:
            send(dsend, d.at[mine], place(dx=a, dz=b), i, step)

    arrived(arecv0, 0)
    total0 = summed(own0, arecv0)
    squares0 = stat_of(total0[:, 384:], 0)
    scale0 = lax.rsqrt(squares0 / D + EPS)
    mixed, parts = attend(0, total0[:, :448] * scale0)
    send_mixed(mixed, b0, 1)
    wrote = [update_state(0, parts)]

    for copy in exchanged:
        copy.wait_recv()

    def project_tokens():
        out = None
        for half in range(2):
            wide = x0[half].reshape(NY * ROWS, 256).astype(F32)
            normed = (wide * pre[half, 1:2, :]).astype(BF16)
            term = project(normed, w1.at[half])
            out = term if out is None else out + term
        return out

    from_tokens = project_tokens()
    p1send[...] = from_tokens.astype(BF16).reshape(NY, ROWS, 512)
    own_tokens = from_tokens[:ROWS]

    arrived(b0.at[pl.ds(1, NY - 1)], 1)
    project_out_here(b0, csend0)
    pl.semaphore_wait(ready, NZ - 1)
    send_sums(csend0, crecv0, 2)
    send_along_y(p1send, p1recv, 4)
    for a in Y_STEPS:
        send(wo1.at[0, c], wo1.at[a, c], place(dy=a), 8, step)
    arrived(crecv0, 2)
    send_rows(summed(csend0[z * NX + x].astype(F32), crecv0).astype(BF16), dsend0, d0, 3)
    arrived(p1recv, 4)
    total_tokens = summed(own_tokens, p1recv)

    arrived(d0.at[pl.ds(0, NX * NZ - 1)], 3)
    half_rows = 2 * NZ
    given = [send(d0.at[pl.ds(half_rows * other, half_rows)], dpart, partner, 7, swap)]
    out = jnp.zeros((NY * ROWS, 512), F32)
    squares_out = cross = squares_step = jnp.zeros((NY * ROWS, 1), F32)
    for half in range(2):
        rows = [
            d0[pl.ds(NZ * (2 * half + part), NZ)].reshape(NZ * ROWS, 128).astype(F32) for part in range(2)
        ]
        rows = jnp.concatenate(rows, axis=1)
        moved = rows * post[half, 0:1, :]
        wide = x0[half].reshape(NY * ROWS, 256).astype(F32)
        squares_out += jnp.sum(rows * rows, axis=1, keepdims=True)
        cross += jnp.sum(wide * moved, axis=1, keepdims=True)
        squares_step += jnp.sum(moved * moved, axis=1, keepdims=True)
        normed = (moved * pre[half, 1:2, :]).astype(BF16)
        out += project(normed, w1.at[half])
    own = jnp.concatenate(
        [out[:, :384], with_columns(out[:, 384:], split_columns([squares_out, cross, squares_step]))], axis=1
    )
    asend1[...] = own.astype(BF16).reshape(NY, ROWS, 512)
    send_along_y(asend1, arecv1, 5)
    own1 = own[:ROWS]
    gathered_out = wo1.at[pl.ds(1, NY - 1), c]
    arrived(gathered_out, 8)
    given.append(send(gathered_out, gathered_out, partner, 8, swap))
    arrived(arecv1, 5)
    total1 = summed(own1, arecv1)
    tail = total1[:, 384:]
    step_scale = lax.rsqrt(stat_of(tail, 0) / D + EPS)
    squares1 = squares0 + step_scale * (2.0 * stat_of(tail, 1) + step_scale * stat_of(tail, 2))
    scale1 = lax.rsqrt(jnp.maximum(squares1, 0.0) / D + EPS)
    mixed, parts = attend(1, (total_tokens[:, :448] + step_scale * total1[:, :448]) * scale1)
    for copy in given:
        copy.wait_recv()
    project_out_all(mixed, csend1)
    send_sums(csend1, crecv1, 6)

    def send_over_chips(source, target, i):
        for k in Y_STEPS + [0]:
            for r in range(2):
                if r == 0 and k == 0:
                    continue
                device = {"tp": tp, "dp": lax.rem(y + NY - k, NY) * 2 + (other if r else c)}
                send(source(r * NY + k), target.at[r * NY + k], device, i, step)

    own_scale = jnp.broadcast_to(step_scale, (ROWS, 128))
    ssend[...] = own_scale
    srecv[0] = own_scale
    send_over_chips(lambda slot: ssend, srecv, 9)
    wrote.append(update_state(1, parts))
    arrived(crecv1, 6)
    send_rows(summed(csend1[z * NX + x].astype(F32), crecv1).astype(BF16), dsend1, d1, 7)

    arrived(srecv.at[pl.ds(1, 2 * NY - 1)], 9)
    for r in range(2):
        for k in range(NY):
            a = (NY - k) % NY
            for part in range(2):
                cols = pl.ds(128 * part, 128)
                rows = dpart[NZ * part + a] if r else d0[half_rows * c + NZ * part + a]
                base[r * NY + k, :, cols] = (
                    tok[other if r else c, a, :, cols].astype(F32)
                    + rows.astype(F32) * srecv[r * NY + k] * post[c, 0:1, cols]
                )

    arrived(d1.at[pl.ds(0, NX * NZ - 1)], 7)
    squares_last = jnp.zeros((ROWS, 128), F32)
    for slot in range(NX * NZ):
        rows = d1[slot].astype(F32)
        squares_last += rows * rows
    last_scale = lax.rsqrt(jnp.sum(squares_last, axis=1, keepdims=True) / D + EPS)
    for r in range(2):
        for k in range(NY):
            for part in range(2):
                rows = d1[half_rows * (other if r else c) + NZ * part + k].astype(F32)
                esend[r * NY + k, :, pl.ds(128 * part, 128)] = (rows * last_scale).astype(BF16)
    erecv[0] = esend[0]
    send_over_chips(lambda slot: esend.at[slot], erecv, 10)
    arrived(erecv.at[pl.ds(1, 2 * NY - 1)], 10)
    for r in range(2):
        for k in range(NY):
            value = base[r * NY + k] + erecv[r * NY + k].astype(F32) * post[c, 1:2, :]
            hout[lax.rem(y + k, NY), other if r else c] = value.astype(BF16)
    copy = pltpu.make_async_copy(hout, hid_hbm, outs.at[2])
    copy.start()
    wrote.append(copy)

    partial.wait_send()
    for copy in exchanged + given:
        copy.wait_send()
    for ref, i in (
        (arecv0, 0), (arecv1, 5), (p1recv, 4), (b0.at[pl.ds(1, NY - 1)], 1), (gathered_out, 8), (crecv0, 2), (crecv1, 6),
        (d0.at[pl.ds(0, NX * NZ - 1)], 3), (d1.at[pl.ds(0, NX * NZ - 1)], 7), (srecv.at[pl.ds(1, 2 * NY - 1)], 9),
        (erecv.at[pl.ds(1, 2 * NY - 1)], 10),
    ):
        sent(ref, i)
    for copy in wrote:
        copy.wait()


def local(tokens, recurrent_state, pre_gain, w_query, w_key, w_value, w_gate, w_decay, decay_bias, head_gain, w_out, post_gain):
    vmem = pltpu.VMEM
    dma = pltpu.SemaphoreType.DMA
    blocks = NX * NZ
    hidden, state = pl.pallas_call(
        kernel,
        out_shape=(
            jax.ShapeDtypeStruct((NY, 2, ROWS, 256), BF16),
            jax.ShapeDtypeStruct((2, ROWS, VAL * KEY), F32),
        ),
        in_specs=[pl.BlockSpec(memory_space=pltpu.HBM)] * 12,
        out_specs=[pl.BlockSpec(memory_space=pl.ANY)] * 2,
        scratch_shapes=[
            vmem((2, NY, ROWS, 256), BF16),
            vmem((2, NY, ROWS, 256), BF16),
            vmem((2, ROWS, VAL * KEY), F32),
            vmem((2, 2, 256), F32),
            vmem((2, 2, 256), F32),
            vmem((2, KEY), F32),
            vmem((2, VAL), F32),
            vmem((2, 256, 256), BF16),
            vmem((2, 2, 256, 256), BF16),
            vmem((2, 128, 256), BF16),
            vmem((NY, 2, 128, 256), BF16),
            vmem((NY * ROWS, 512), BF16),
            vmem((NY * ROWS, 512), BF16),
            vmem((NY, ROWS, 512), BF16),
            vmem((NY - 1, ROWS, 512), BF16),
            vmem((NY, ROWS, 512), BF16),
            vmem((NY - 1, ROWS, 512), BF16),
            vmem((NY, ROWS, 512), BF16),
            vmem((NY - 1, ROWS, 512), BF16),
            vmem((NY, ROWS, 128), BF16),
            vmem((blocks, ROWS, 128), BF16),
            vmem((blocks, ROWS, 128), BF16),
            vmem((blocks - 1, ROWS, 128), BF16),
            vmem((blocks - 1, ROWS, 128), BF16),
            vmem((ROWS, 128), BF16),
            vmem((ROWS, 128), BF16),
            vmem((blocks, ROWS, 128), BF16),
            vmem((blocks, ROWS, 128), BF16),
            vmem((2 * NZ, ROWS, 128), BF16),
            vmem((ROWS, 128), F32),
            vmem((2 * NY, ROWS, 128), F32),
            vmem((2 * NY, ROWS, 256), F32),
            vmem((2 * NY, ROWS, 256), BF16),
            vmem((2 * NY, ROWS, 256), BF16),
            vmem((NY, 2, ROWS, 256), BF16),
            dma((18,)),
            dma((9,)),
            dma((9,)),
            dma((11,)),
            dma((11,)),
            pltpu.SemaphoreType.REGULAR,
            dma((3,)),
        ],
        compiler_params=pltpu.CompilerParams(
            collective_id=0, has_side_effects=True, vmem_limit_bytes=32 * 1024 * 1024
        ),
    )(
        *(pltpu.with_memory_space_constraint(v, pltpu.HBM) for v in (
        tokens.reshape(NY, 2, ROWS, 256), recurrent_state, pre_gain, jnp.swapaxes(w_query, 1, 2),
        jnp.swapaxes(w_key, 1, 2), w_value, w_gate, jnp.swapaxes(w_decay, 1, 2),
        decay_bias, head_gain, w_out, post_gain,))
    )
    return hidden.reshape(NY * 2 * ROWS, 256), state


def solution(mesh):
    in_specs = (
        P(None, "dp"), P(None, "dp", "tp"), P(None, "dp"), P(None, "dp", "tp"), P(None, "dp", "tp"),
        P(None, "dp", "tp"), P(None, "dp", "tp"), P(None, "dp", "tp"), P(None, "tp"), P(), P(None, "tp", "dp"),
        P(None, "dp"),
    )
    out_specs = (P(None, "dp"), P(None, "dp", "tp"))
    return jax.shard_map(local, mesh=mesh, in_specs=in_specs, out_specs=out_specs, check_vma=False)
```

```python
import jax
import jax.numpy as jnp
from jax import lax
from jax.experimental import pallas as pl
from jax.experimental.pallas import tpu as pltpu
from jax.sharding import PartitionSpec as P

MESH = pl.DeviceIdType.MESH
D = 4096
KEY = 64
VAL = 128
NX, NY, NZ = 4, 8, 8
ROWS = 16
EPS = 1e-6
F32 = jnp.float32
BF16 = jnp.bfloat16


def ring(step, size):
    return min(step, size - step)


Y_STEPS = sorted(range(1, NY), key=lambda a: -ring(a, NY))
XZ_STEPS = sorted(
    ((a, b) for a in range(NX) for b in range(NZ) if a or b),
    key=lambda s: -ring(s[0], NX) - ring(s[1], NZ),
)


def lanes(shape):
    return lax.broadcasted_iota(jnp.int32, shape, 1)


def halves(value):
    high = value.astype(BF16)
    return high.astype(F32), (value - high.astype(F32))


def with_columns(tile, columns):
    at = lanes(tile.shape)
    for place, column in columns:
        tile = jnp.where(at == place, column, tile)
    return tile


def split_columns(stats):
    columns = []
    for i, stat in enumerate(stats):
        high, low = halves(stat)
        columns += [(KEY + 2 * i, high), (KEY + 2 * i + 1, low)]
    return columns


def stat_of(tile, i):
    return tile[:, KEY + 2 * i : KEY + 2 * i + 1] + tile[:, KEY + 2 * i + 1 : KEY + 2 * i + 2]


def kernel(
    tok_hbm, state_hbm, pre_hbm, wq_hbm, wk_hbm, wv_hbm, wg_hbm, wd_hbm, bias_hbm, hgain_hbm, wo_hbm, post_hbm,
    hout, snew,
    tok, x0, state, pre, post, bias, hgain, w0, w1, wo0, wo1,
    psend, precv, asend0, arecv0, asend1, arecv1, p1send, p1recv,
    b0, csend0, csend1, crecv0, crecv1, dsend0, dsend1, d0, d1, dpart,
    ssend, srecv, base, esend, erecv,
    load, xsend, xrecv, phase_send, phase_recv, ready,
):
    tp, dp = lax.axis_index("tp"), lax.axis_index("dp")
    z, x = tp // NX, lax.rem(tp, NX)
    y, c = dp // 2, lax.rem(dp, 2)
    other = 1 - c

    def place(dx=0, dy=0, dz=0):
        return {
            "tp": lax.rem(z + dz, NZ) * NX + lax.rem(x + dx, NX),
            "dp": lax.rem(y + dy, NY) * 2 + c,
        }

    partner = {"tp": tp, "dp": y * 2 + other}

    barrier = pltpu.get_barrier_semaphore()
    for a in Y_STEPS:
        pl.semaphore_signal(barrier, inc=1, device_id=place(dy=a), device_id_type=MESH)
    for a in range(1, NZ):
        pl.semaphore_signal(barrier, inc=1, device_id=place(dz=a), device_id_type=MESH)
    for a in range(1, NX):
        pl.semaphore_signal(barrier, inc=1, device_id=place(dx=a), device_id_type=MESH)
    pl.semaphore_signal(barrier, inc=1, device_id=partner, device_id_type=MESH)

    def fetch(source, target, i):
        copy = pltpu.make_async_copy(source, target, load.at[i])
        copy.start()
        return copy

    def fetch_weights(section, target, i):
        return [
            fetch(wv_hbm.at[section], target.at[0, :, pl.ds(0, 128)], i),
            fetch(wg_hbm.at[section], target.at[0, :, pl.ds(128, 128)], i + 1),
            fetch(wq_hbm.at[section], target.at[1, pl.ds(0, KEY)], i + 2),
            fetch(wk_hbm.at[section], target.at[1, pl.ds(KEY, KEY)], i + 3),
            fetch(wd_hbm.at[section], target.at[1, pl.ds(2 * KEY, KEY)], i + 4),
        ]

    def project(rows, weights):
        return jnp.concatenate(
            [
                jnp.dot(rows, weights[0], preferred_element_type=F32),
                lax.dot_general(rows, weights[1], (((1,), (1,)), ((), ())), preferred_element_type=F32),
            ],
            axis=1,
        )

    for a in range(NY):
        pltpu.make_async_copy(tok_hbm.at[lax.rem(y + NY - a, NY)], tok.at[:, a], load.at[0]).start()
    first = [
        fetch(pre_hbm, pre.at[c], 1),
        *fetch_weights(0, w0, 2),
    ]
    second = [
        fetch(post_hbm, post.at[c], 7),
        *fetch_weights(1, w1.at[c], 8),
        fetch(wo_hbm.at[0], wo0.at[c], 13),
        fetch(wo_hbm.at[1], wo1.at[0, c], 17),
        fetch(bias_hbm, bias, 14),
        fetch(hgain_hbm, hgain, 15),
    ]
    third = [fetch(state_hbm, state, 16)]

    pltpu.make_async_copy(tok, tok, load.at[0]).wait()
    for copy in first:
        copy.wait()
    w0[1, 3 * KEY :] = jnp.zeros((KEY, 256), BF16)

    def project_first(half):
        wide = tok[half].reshape(NY * ROWS, 256).astype(F32)
        normed = (wide * pre[c, 0:1, :]).astype(BF16)
        out = project(normed, w0)
        squares = jnp.sum(wide * wide, axis=1, keepdims=True)
        return jnp.concatenate(
            [out[:, :384], with_columns(out[:, 384:], split_columns([squares]))], axis=1
        )

    psend[...] = project_first(other).astype(BF16)
    own = project_first(c)
    pl.semaphore_wait(barrier, 1 + (NY - 1) + (NZ - 1) + (NX - 1))

    def send(source, target, device, i, sems):
        copy = pltpu.make_async_remote_copy(
            src_ref=source, dst_ref=target, send_sem=sems[0].at[i], recv_sem=sems[1].at[i],
            device_id=device, device_id_type=MESH,
        )
        copy.start()
        return copy

    swap = (xsend, xrecv)
    partial = send(psend, precv, partner, 0, swap)
    for a in range(1, NZ):
        pl.semaphore_signal(ready, inc=1, device_id=place(dz=a), device_id_type=MESH)

    step = (phase_send, phase_recv)

    def send_along_y(source, target, i):
        for a in Y_STEPS:
            send(source.at[a], target.at[a - 1], place(dy=NY - a), i, step)

    def arrived(ref, i):
        pltpu.make_async_copy(ref, ref, phase_recv.at[i]).wait()

    def sent(ref, i):
        pltpu.make_async_copy(ref, ref, phase_send.at[i]).wait()

    partial.wait_recv()
    own = own + precv[...].astype(F32)
    asend0[...] = own.astype(BF16).reshape(NY, ROWS, 512)
    send_along_y(asend0, arecv0, 0)
    own0 = own[:ROWS]

    for copy in second:
        copy.wait()
    w1[c, 1, 3 * KEY :] = jnp.zeros((KEY, 256), BF16)
    exchanged = [
        send(tok.at[other], x0.at[c], partner, 1, swap),
        send(pre.at[c], pre.at[c], partner, 2, swap),
        send(post.at[c], post.at[c], partner, 3, swap),
        send(wo0.at[c], wo0.at[c], partner, 4, swap),
        send(wo1.at[0, c], wo1.at[0, c], partner, 6, swap),
        send(w1.at[c], w1.at[c], partner, 5, swap),
    ]
    x0[c] = tok[c]
    for copy in third:
        copy.wait()

    def summed(own_rows, ref):
        total = own_rows
        for i in range(ref.shape[0]):
            total = total + ref[i].astype(F32)
        return total

    lane = lanes((ROWS, 128))
    half_sum = (
        lax.broadcasted_iota(jnp.int32, (128, 128), 0) // KEY == lax.rem(lanes((128, 128)), 2)
    ).astype(F32).astype(BF16)

    def attend(section, proj):
        values, gate = proj[:, 0:128], proj[:, 128:256]
        query = proj[:, 256:320].astype(BF16).astype(F32)
        key = proj[:, 320:384].astype(BF16).astype(F32)
        pre_decay = proj[:, 384:448] + bias[section : section + 1, :]
        log_sigmoid = jnp.minimum(pre_decay, 0.0) - jnp.log(1.0 + jnp.exp(-jnp.abs(pre_decay)))
        decay = jnp.exp(log_sigmoid / 16.0)
        faded = query * decay
        faded2 = jnp.concatenate([faded, faded], axis=1)
        terms = jnp.concatenate(
            [state[section, :, 128 * j : 128 * (j + 1)] * faded2 for j in range(KEY)], axis=0
        )
        high = terms.astype(BF16)
        low = (terms - high.astype(F32)).astype(BF16)
        sums = jnp.dot(high, half_sum, preferred_element_type=F32) + jnp.dot(
            low, half_sum, preferred_element_type=F32
        )
        old_part = jnp.zeros((ROWS, 128), F32)
        for j in range(KEY):
            old_part = jnp.where(lane // 2 == j, sums[ROWS * j : ROWS * (j + 1)], old_part)
        readout = (old_part + values * jnp.sum(query * key, axis=1, keepdims=True)) * KEY**-0.5
        mean = jnp.mean(readout * readout, axis=1, keepdims=True)
        gated = gate / (1.0 + jnp.exp(-gate))
        mixed = readout * lax.rsqrt(mean + EPS) * hgain[section : section + 1, :] * gated
        return mixed.astype(BF16), (values, key, decay)

    def update_state(section, parts):
        values, key, decay = parts
        decay2 = jnp.concatenate([decay, decay], axis=1)
        key2 = jnp.concatenate([key, key], axis=1)
        for j in range(KEY):
            value = jnp.where(lane < KEY, values[:, 2 * j : 2 * j + 1], values[:, 2 * j + 1 : 2 * j + 2])
            tile = pl.ds(128 * j, 128)
            snew[section, :, tile] = decay2 * state[section, :, tile] + key2 * value

    def send_mixed(mixed, b, i):
        b[0] = mixed
        for a in Y_STEPS:
            send(b.at[0], b.at[a], place(dy=a), i, step)

    def project_out_here(b, csend):
        gathered = b[...].reshape(NY * ROWS, 128)
        for half in range(2):
            out = jnp.dot(gathered, wo0[half], preferred_element_type=F32).astype(BF16)
            for zz in range(NZ):
                for part in range(2):
                    csend[zz * NX + half * 2 + part] = out[ROWS * zz : ROWS * (zz + 1), 128 * part : 128 * (part + 1)]

    def project_out_all(mixed, csend):
        for back in range(NY):
            for half in range(2):
                out = jnp.dot(mixed, wo1[back, half], preferred_element_type=F32).astype(BF16)
                for part in range(2):
                    csend[back * NX + half * 2 + part] = out[:, 128 * part : 128 * (part + 1)]

    def send_sums(csend, crecv, i):
        for n, (a, b) in enumerate(XZ_STEPS):
            block = lax.rem(z + b, NZ) * NX + lax.rem(x + a, NX)
            send(csend.at[block], crecv.at[n], place(dx=a, dz=b), i, step)

    def send_rows(rows, dsend, d, i):
        mine = x * NZ + z
        dsend[...] = rows
        d[mine] = rows
        for a, b in XZ_STEPS:
            send(dsend, d.at[mine], place(dx=a, dz=b), i, step)

    arrived(arecv0, 0)
    total0 = summed(own0, arecv0)
    squares0 = stat_of(total0[:, 384:], 0)
    scale0 = lax.rsqrt(squares0 / D + EPS)
    mixed, parts = attend(0, total0[:, :448] * scale0)
    send_mixed(mixed, b0, 1)
    update_state(0, parts)

    for copy in exchanged:
        copy.wait_recv()

    def project_tokens():
        out = None
        for half in range(2):
            wide = x0[half].reshape(NY * ROWS, 256).astype(F32)
            normed = (wide * pre[half, 1:2, :]).astype(BF16)
            term = project(normed, w1.at[half])
            out = term if out is None else out + term
        return out

    from_tokens = project_tokens()
    p1send[...] = from_tokens.astype(BF16).reshape(NY, ROWS, 512)
    own_tokens = from_tokens[:ROWS]
    send_along_y(p1send, p1recv, 4)

    arrived(b0.at[pl.ds(1, NY - 1)], 1)
    project_out_here(b0, csend0)
    pl.semaphore_wait(ready, NZ - 1)
    send_sums(csend0, crecv0, 2)
    for a in (2, NY - 2, 1, NY - 1):
        send(wo1.at[0, c], wo1.at[a, c], place(dy=a), 8, step)
    arrived(crecv0, 2)
    send_rows(summed(csend0[z * NX + x].astype(F32), crecv0).astype(BF16), dsend0, d0, 3)
    arrived(wo1.at[pl.ds(0, 4), c], 8)
    front, back = pl.ds(0, 64), pl.ds(64, 64)
    send(wo1.at[2, c, front], wo1.at[4, c, front], place(dy=2), 11, step)
    send(wo1.at[6, c, back], wo1.at[4, c, back], place(dy=NY - 2), 11, step)
    send(wo1.at[2, c], wo1.at[3, c], place(dy=1), 11, step)
    send(wo1.at[6, c], wo1.at[5, c], place(dy=NY - 1), 11, step)
    near, far, rest = (wo1.at[pl.ds(first, count), c] for first, count in ((1, 2), (6, 2), (3, 3)))
    given = [send(near, near, partner, 8, swap), send(far, far, partner, 9, swap)]
    arrived(p1recv, 4)
    total_tokens = summed(own_tokens, p1recv)

    arrived(d0.at[pl.ds(0, NX * NZ - 1)], 3)
    half_rows = 2 * NZ
    given.append(send(d0.at[pl.ds(half_rows * other, half_rows)], dpart, partner, 7, swap))
    out = jnp.zeros((NY * ROWS, 512), F32)
    squares_out = cross = squares_step = jnp.zeros((NY * ROWS, 1), F32)
    for half in range(2):
        rows = [
            d0[pl.ds(NZ * (2 * half + part), NZ)].reshape(NZ * ROWS, 128).astype(F32) for part in range(2)
        ]
        rows = jnp.concatenate(rows, axis=1)
        moved = rows * post[half, 0:1, :]
        wide = x0[half].reshape(NY * ROWS, 256).astype(F32)
        squares_out += jnp.sum(rows * rows, axis=1, keepdims=True)
        cross += jnp.sum(wide * moved, axis=1, keepdims=True)
        squares_step += jnp.sum(moved * moved, axis=1, keepdims=True)
        normed = (moved * pre[half, 1:2, :]).astype(BF16)
        out += project(normed, w1.at[half])
    own = jnp.concatenate(
        [out[:, :384], with_columns(out[:, 384:], split_columns([squares_out, cross, squares_step]))], axis=1
    )
    asend1[...] = own.astype(BF16).reshape(NY, ROWS, 512)
    send_along_y(asend1, arecv1, 5)
    own1 = own[:ROWS]
    arrived(rest, 11)
    given.append(send(rest, rest, partner, 10, swap))
    arrived(arecv1, 5)
    total1 = summed(own1, arecv1)
    tail = total1[:, 384:]
    step_scale = lax.rsqrt(stat_of(tail, 0) / D + EPS)
    squares1 = squares0 + step_scale * (2.0 * stat_of(tail, 1) + step_scale * stat_of(tail, 2))
    scale1 = lax.rsqrt(jnp.maximum(squares1, 0.0) / D + EPS)
    mixed, parts = attend(1, (total_tokens[:, :448] + step_scale * total1[:, :448]) * scale1)
    for copy in given:
        copy.wait_recv()
    project_out_all(mixed, csend1)
    send_sums(csend1, crecv1, 6)

    def send_over_chips(source, target, i):
        for k in Y_STEPS + [0]:
            for r in range(2):
                if r == 0 and k == 0:
                    continue
                device = {"tp": tp, "dp": lax.rem(y + NY - k, NY) * 2 + (other if r else c)}
                send(source(r * NY + k), target.at[r * NY + k], device, i, step)

    own_scale = jnp.broadcast_to(step_scale, (ROWS, 128))
    ssend[...] = own_scale
    srecv[0] = own_scale
    send_over_chips(lambda slot: ssend, srecv, 9)
    update_state(1, parts)
    arrived(crecv1, 6)
    send_rows(summed(csend1[z * NX + x].astype(F32), crecv1).astype(BF16), dsend1, d1, 7)

    arrived(srecv.at[pl.ds(1, 2 * NY - 1)], 9)
    for r in range(2):
        for k in range(NY):
            a = (NY - k) % NY
            for part in range(2):
                cols = pl.ds(128 * part, 128)
                rows = dpart[NZ * part + a] if r else d0[half_rows * c + NZ * part + a]
                base[r * NY + k, :, cols] = (
                    tok[other if r else c, a, :, cols].astype(F32)
                    + rows.astype(F32) * srecv[r * NY + k] * post[c, 0:1, cols]
                )

    arrived(d1.at[pl.ds(0, NX * NZ - 1)], 7)
    squares_last = jnp.zeros((ROWS, 128), F32)
    for slot in range(NX * NZ):
        rows = d1[slot].astype(F32)
        squares_last += rows * rows
    last_scale = lax.rsqrt(jnp.sum(squares_last, axis=1, keepdims=True) / D + EPS)
    for r in range(2):
        for k in range(NY):
            for part in range(2):
                rows = d1[half_rows * (other if r else c) + NZ * part + k].astype(F32)
                esend[r * NY + k, :, pl.ds(128 * part, 128)] = (rows * last_scale).astype(BF16)
    erecv[0] = esend[0]
    send_over_chips(lambda slot: esend.at[slot], erecv, 10)
    arrived(erecv.at[pl.ds(1, 2 * NY - 1)], 10)
    for r in range(2):
        for k in range(NY):
            value = base[r * NY + k] + erecv[r * NY + k].astype(F32) * post[c, 1:2, :]
            hout[lax.rem(y + k, NY), other if r else c] = value.astype(BF16)
    partial.wait_send()
    for copy in exchanged + given:
        copy.wait_send()
    for ref, i in (
        (arecv0, 0), (arecv1, 5), (p1recv, 4), (b0.at[pl.ds(1, NY - 1)], 1), (wo1.at[pl.ds(0, 4), c], 8), (rest, 11), (crecv0, 2), (crecv1, 6),
        (d0.at[pl.ds(0, NX * NZ - 1)], 3), (d1.at[pl.ds(0, NX * NZ - 1)], 7), (srecv.at[pl.ds(1, 2 * NY - 1)], 9),
        (erecv.at[pl.ds(1, 2 * NY - 1)], 10),
    ):
        sent(ref, i)


def write_out(hidden, state, hidden_out, state_out, done):
    copies = [
        pltpu.make_async_copy(state, state_out, done.at[0]),
        pltpu.make_async_copy(hidden, hidden_out, done.at[1]),
    ]
    for copy in copies:
        copy.start()
    for copy in copies:
        copy.wait()


def local(tokens, recurrent_state, pre_gain, w_query, w_key, w_value, w_gate, w_decay, decay_bias, head_gain, w_out, post_gain):
    vmem = pltpu.VMEM
    dma = pltpu.SemaphoreType.DMA
    blocks = NX * NZ
    hidden, state = pl.pallas_call(
        kernel,
        out_shape=(
            jax.ShapeDtypeStruct((NY, 2, ROWS, 256), BF16),
            jax.ShapeDtypeStruct((2, ROWS, VAL * KEY), F32),
        ),
        in_specs=[pl.BlockSpec(memory_space=pltpu.HBM)] * 12,
        out_specs=[pl.BlockSpec(memory_space=pltpu.VMEM)] * 2,
        scratch_shapes=[
            vmem((2, NY, ROWS, 256), BF16),
            vmem((2, NY, ROWS, 256), BF16),
            vmem((2, ROWS, VAL * KEY), F32),
            vmem((2, 2, 256), F32),
            vmem((2, 2, 256), F32),
            vmem((2, KEY), F32),
            vmem((2, VAL), F32),
            vmem((2, 256, 256), BF16),
            vmem((2, 2, 256, 256), BF16),
            vmem((2, 128, 256), BF16),
            vmem((NY, 2, 128, 256), BF16),
            vmem((NY * ROWS, 512), BF16),
            vmem((NY * ROWS, 512), BF16),
            vmem((NY, ROWS, 512), BF16),
            vmem((NY - 1, ROWS, 512), BF16),
            vmem((NY, ROWS, 512), BF16),
            vmem((NY - 1, ROWS, 512), BF16),
            vmem((NY, ROWS, 512), BF16),
            vmem((NY - 1, ROWS, 512), BF16),
            vmem((NY, ROWS, 128), BF16),
            vmem((blocks, ROWS, 128), BF16),
            vmem((blocks, ROWS, 128), BF16),
            vmem((blocks - 1, ROWS, 128), BF16),
            vmem((blocks - 1, ROWS, 128), BF16),
            vmem((ROWS, 128), BF16),
            vmem((ROWS, 128), BF16),
            vmem((blocks, ROWS, 128), BF16),
            vmem((blocks, ROWS, 128), BF16),
            vmem((2 * NZ, ROWS, 128), BF16),
            vmem((ROWS, 128), F32),
            vmem((2 * NY, ROWS, 128), F32),
            vmem((2 * NY, ROWS, 256), F32),
            vmem((2 * NY, ROWS, 256), BF16),
            vmem((2 * NY, ROWS, 256), BF16),
            dma((18,)),
            dma((11,)),
            dma((11,)),
            dma((12,)),
            dma((12,)),
            pltpu.SemaphoreType.REGULAR,
        ],
        compiler_params=pltpu.CompilerParams(
            collective_id=0, has_side_effects=True, vmem_limit_bytes=32 * 1024 * 1024
        ),
    )(
        *(pltpu.with_memory_space_constraint(v, pltpu.HBM) for v in (
        tokens.reshape(NY, 2, ROWS, 256), recurrent_state, pre_gain, jnp.swapaxes(w_query, 1, 2),
        jnp.swapaxes(w_key, 1, 2), w_value, w_gate, jnp.swapaxes(w_decay, 1, 2),
        decay_bias, head_gain, w_out, post_gain,))
    )
    hidden, state = pl.pallas_call(
        write_out,
        out_shape=(jax.ShapeDtypeStruct(hidden.shape, BF16), jax.ShapeDtypeStruct(state.shape, F32)),
        in_specs=[pl.BlockSpec(memory_space=pl.ANY)] * 2,
        out_specs=[pl.BlockSpec(memory_space=pl.ANY)] * 2,
        scratch_shapes=[dma((2,))],
        compiler_params=pltpu.CompilerParams(vmem_limit_bytes=1024 * 1024),
    )(hidden, state)
    return hidden.reshape(NY * 2 * ROWS, 256), state


def solution(mesh):
    in_specs = (
        P(None, "dp"), P(None, "dp", "tp"), P(None, "dp"), P(None, "dp", "tp"), P(None, "dp", "tp"),
        P(None, "dp", "tp"), P(None, "dp", "tp"), P(None, "dp", "tp"), P(None, "tp"), P(), P(None, "tp", "dp"),
        P(None, "dp"),
    )
    out_specs = (P(None, "dp"), P(None, "dp", "tp"))
    return jax.shard_map(local, mesh=mesh, in_specs=in_specs, out_specs=out_specs, check_vma=False)
```

```python
import jax
import jax.numpy as jnp
from jax import lax
from jax.experimental import pallas as pl
from jax.experimental.pallas import tpu as pltpu
from jax.sharding import PartitionSpec as P

MESH = pl.DeviceIdType.MESH
D = 4096
KEY = 64
VAL = 128
NX, NY, NZ = 4, 8, 8
ROWS = 16
EPS = 1e-6
F32 = jnp.float32
BF16 = jnp.bfloat16


def ring(step, size):
    return min(step, size - step)


Y_STEPS = sorted(range(1, NY), key=lambda a: -ring(a, NY))
XZ_STEPS = sorted(
    ((a, b) for a in range(NX) for b in range(NZ) if a or b),
    key=lambda s: (-ring(s[0], NX) - ring(s[1], NZ), -ring(s[0], NX)),
)


def lanes(shape):
    return lax.broadcasted_iota(jnp.int32, shape, 1)


def halves(value):
    high = value.astype(BF16)
    return high.astype(F32), (value - high.astype(F32))


def with_columns(tile, columns):
    at = lanes(tile.shape)
    for place, column in columns:
        tile = jnp.where(at == place, column, tile)
    return tile


def split_columns(stats):
    columns = []
    for i, stat in enumerate(stats):
        high, low = halves(stat)
        columns += [(KEY + 2 * i, high), (KEY + 2 * i + 1, low)]
    return columns


def stat_of(tile, i):
    return tile[:, KEY + 2 * i : KEY + 2 * i + 1] + tile[:, KEY + 2 * i + 1 : KEY + 2 * i + 2]


def kernel(
    tok_hbm, state_hbm, pre_hbm, wq_hbm, wk_hbm, wv_hbm, wg_hbm, wd_hbm, bias_hbm, hgain_hbm, wo_hbm, post_hbm,
    hout, snew,
    tok, x0, state, pre, post, bias, hgain, w0, w1, wo0, wo1,
    psend, precv, asend0, arecv0, asend1, arecv1, p1send, p1recv,
    b0, csend0, csend1, crecv0, crecv1, dsend0, dsend1, d0, d1, dpart,
    ssend, srecv, base, esend, erecv,
    load, xsend, xrecv, phase_send, phase_recv, ready,
):
    tp, dp = lax.axis_index("tp"), lax.axis_index("dp")
    z, x = tp // NX, lax.rem(tp, NX)
    y, c = dp // 2, lax.rem(dp, 2)
    other = 1 - c

    def place(dx=0, dy=0, dz=0):
        return {
            "tp": lax.rem(z + dz, NZ) * NX + lax.rem(x + dx, NX),
            "dp": lax.rem(y + dy, NY) * 2 + c,
        }

    partner = {"tp": tp, "dp": y * 2 + other}

    barrier = pltpu.get_barrier_semaphore()
    for a in Y_STEPS:
        pl.semaphore_signal(barrier, inc=1, device_id=place(dy=a), device_id_type=MESH)
    for a in range(1, NZ):
        pl.semaphore_signal(barrier, inc=1, device_id=place(dz=a), device_id_type=MESH)
    for a in range(1, NX):
        pl.semaphore_signal(barrier, inc=1, device_id=place(dx=a), device_id_type=MESH)
    pl.semaphore_signal(barrier, inc=1, device_id=partner, device_id_type=MESH)

    def fetch(source, target, i):
        copy = pltpu.make_async_copy(source, target, load.at[i])
        copy.start()
        return copy

    def fetch_weights(section, target, i):
        return [
            fetch(wv_hbm.at[section], target.at[0, :, pl.ds(0, 128)], i),
            fetch(wg_hbm.at[section], target.at[0, :, pl.ds(128, 128)], i + 1),
            fetch(wq_hbm.at[section], target.at[1, pl.ds(0, KEY)], i + 2),
            fetch(wk_hbm.at[section], target.at[1, pl.ds(KEY, KEY)], i + 3),
            fetch(wd_hbm.at[section], target.at[1, pl.ds(2 * KEY, KEY)], i + 4),
        ]

    def project(rows, weights):
        return jnp.concatenate(
            [
                jnp.dot(rows, weights[0], preferred_element_type=F32),
                lax.dot_general(rows, weights[1], (((1,), (1,)), ((), ())), preferred_element_type=F32),
            ],
            axis=1,
        )

    for a in range(NY):
        pltpu.make_async_copy(tok_hbm.at[lax.rem(y + NY - a, NY)], tok.at[:, a], load.at[0]).start()
    first = [
        fetch(pre_hbm, pre.at[c], 1),
        *fetch_weights(0, w0, 2),
    ]
    second = [
        fetch(post_hbm, post.at[c], 7),
        *fetch_weights(1, w1.at[c], 8),
        fetch(wo_hbm.at[0], wo0.at[c], 13),
        fetch(wo_hbm.at[1], wo1.at[0, c], 17),
        fetch(bias_hbm, bias, 14),
        fetch(hgain_hbm, hgain, 15),
    ]
    third = [fetch(state_hbm, state, 16)]

    pltpu.make_async_copy(tok, tok, load.at[0]).wait()
    for copy in first:
        copy.wait()
    w0[1, 3 * KEY :] = jnp.zeros((KEY, 256), BF16)

    def project_first(half):
        wide = tok[half].reshape(NY * ROWS, 256).astype(F32)
        normed = (wide * pre[c, 0:1, :]).astype(BF16)
        out = project(normed, w0)
        squares = jnp.sum(wide * wide, axis=1, keepdims=True)
        return jnp.concatenate(
            [out[:, :384], with_columns(out[:, 384:], split_columns([squares]))], axis=1
        )

    psend[...] = project_first(other).astype(BF16)
    own = project_first(c)
    pl.semaphore_wait(barrier, 1 + (NY - 1) + (NZ - 1) + (NX - 1))

    def send(source, target, device, i, sems):
        copy = pltpu.make_async_remote_copy(
            src_ref=source, dst_ref=target, send_sem=sems[0].at[i], recv_sem=sems[1].at[i],
            device_id=device, device_id_type=MESH,
        )
        copy.start()
        return copy

    swap = (xsend, xrecv)
    partial = send(psend, precv, partner, 0, swap)
    for a in range(1, NZ):
        pl.semaphore_signal(ready, inc=1, device_id=place(dz=a), device_id_type=MESH)

    step = (phase_send, phase_recv)

    def send_along_y(source, target, i):
        for a in Y_STEPS:
            send(source.at[a], target.at[a - 1], place(dy=NY - a), i, step)

    def arrived(ref, i):
        pltpu.make_async_copy(ref, ref, phase_recv.at[i]).wait()

    def sent(ref, i):
        pltpu.make_async_copy(ref, ref, phase_send.at[i]).wait()

    partial.wait_recv()
    own = own + precv[...].astype(F32)
    asend0[...] = own.astype(BF16).reshape(NY, ROWS, 512)
    send_along_y(asend0, arecv0, 0)
    own0 = own[:ROWS]

    for copy in second:
        copy.wait()
    w1[c, 1, 3 * KEY :] = jnp.zeros((KEY, 256), BF16)
    exchanged = [
        send(tok.at[other], x0.at[c], partner, 1, swap),
        send(pre.at[c], pre.at[c], partner, 2, swap),
        send(post.at[c], post.at[c], partner, 3, swap),
        send(wo0.at[c], wo0.at[c], partner, 4, swap),
        send(wo1.at[0, c], wo1.at[0, c], partner, 6, swap),
        send(w1.at[c], w1.at[c], partner, 5, swap),
    ]
    x0[c] = tok[c]
    for copy in third:
        copy.wait()

    def summed(own_rows, ref):
        total = own_rows
        for i in range(ref.shape[0]):
            total = total + ref[i].astype(F32)
        return total

    lane = lanes((ROWS, 128))
    half_sum = (
        lax.broadcasted_iota(jnp.int32, (128, 128), 0) // KEY == lax.rem(lanes((128, 128)), 2)
    ).astype(F32).astype(BF16)

    def attend(section, proj):
        values, gate = proj[:, 0:128], proj[:, 128:256]
        query = proj[:, 256:320].astype(BF16).astype(F32)
        key = proj[:, 320:384].astype(BF16).astype(F32)
        pre_decay = proj[:, 384:448] + bias[section : section + 1, :]
        log_sigmoid = jnp.minimum(pre_decay, 0.0) - jnp.log(1.0 + jnp.exp(-jnp.abs(pre_decay)))
        decay = jnp.exp(log_sigmoid / 16.0)
        faded = query * decay
        faded2 = jnp.concatenate([faded, faded], axis=1)
        terms = jnp.concatenate(
            [state[section, :, 128 * j : 128 * (j + 1)] * faded2 for j in range(KEY)], axis=0
        )
        high = terms.astype(BF16)
        low = (terms - high.astype(F32)).astype(BF16)
        sums = jnp.dot(high, half_sum, preferred_element_type=F32) + jnp.dot(
            low, half_sum, preferred_element_type=F32
        )
        old_part = jnp.zeros((ROWS, 128), F32)
        for j in range(KEY):
            old_part = jnp.where(lane // 2 == j, sums[ROWS * j : ROWS * (j + 1)], old_part)
        readout = (old_part + values * jnp.sum(query * key, axis=1, keepdims=True)) * KEY**-0.5
        mean = jnp.mean(readout * readout, axis=1, keepdims=True)
        gated = gate / (1.0 + jnp.exp(-gate))
        mixed = readout * lax.rsqrt(mean + EPS) * hgain[section : section + 1, :] * gated
        return mixed.astype(BF16), (values, key, decay)

    def update_state(section, parts):
        values, key, decay = parts
        decay2 = jnp.concatenate([decay, decay], axis=1)
        key2 = jnp.concatenate([key, key], axis=1)
        for j in range(KEY):
            value = jnp.where(lane < KEY, values[:, 2 * j : 2 * j + 1], values[:, 2 * j + 1 : 2 * j + 2])
            tile = pl.ds(128 * j, 128)
            snew[section, :, tile] = decay2 * state[section, :, tile] + key2 * value

    def send_mixed(mixed, b, i):
        b[0] = mixed
        for a in Y_STEPS:
            send(b.at[0], b.at[a], place(dy=a), i, step)

    def project_out_here(b, csend):
        gathered = b[...].reshape(NY * ROWS, 128)
        for half in range(2):
            out = jnp.dot(gathered, wo0[half], preferred_element_type=F32).astype(BF16)
            for zz in range(NZ):
                for part in range(2):
                    csend[zz * NX + half * 2 + part] = out[ROWS * zz : ROWS * (zz + 1), 128 * part : 128 * (part + 1)]

    def project_out_all(mixed, csend):
        for back in range(NY):
            for half in range(2):
                out = jnp.dot(mixed, wo1[back, half], preferred_element_type=F32).astype(BF16)
                for part in range(2):
                    csend[back * NX + half * 2 + part] = out[:, 128 * part : 128 * (part + 1)]

    def send_sums(csend, crecv, i):
        for n, (a, b) in enumerate(XZ_STEPS):
            block = lax.rem(z + b, NZ) * NX + lax.rem(x + a, NX)
            send(csend.at[block], crecv.at[n], place(dx=a, dz=b), i, step)

    def send_rows(rows, dsend, d, i):
        mine = x * NZ + z
        dsend[...] = rows
        d[mine] = rows
        for a, b in XZ_STEPS:
            send(dsend, d.at[mine], place(dx=a, dz=b), i, step)

    arrived(arecv0, 0)
    total0 = summed(own0, arecv0)
    squares0 = stat_of(total0[:, 384:], 0)
    scale0 = lax.rsqrt(squares0 / D + EPS)
    mixed, parts = attend(0, total0[:, :448] * scale0)
    send_mixed(mixed, b0, 1)
    update_state(0, parts)

    for copy in exchanged:
        copy.wait_recv()

    def project_tokens():
        out = None
        for half in range(2):
            wide = x0[half].reshape(NY * ROWS, 256).astype(F32)
            normed = (wide * pre[half, 1:2, :]).astype(BF16)
            term = project(normed, w1.at[half])
            out = term if out is None else out + term
        return out

    from_tokens = project_tokens()
    p1send[...] = from_tokens.astype(BF16).reshape(NY, ROWS, 512)
    own_tokens = from_tokens[:ROWS]
    send_along_y(p1send, p1recv, 4)

    arrived(b0.at[pl.ds(1, NY - 1)], 1)
    project_out_here(b0, csend0)
    pl.semaphore_wait(ready, NZ - 1)
    send_sums(csend0, crecv0, 2)
    for a in (2, NY - 2, 1, NY - 1):
        send(wo1.at[0, c], wo1.at[a, c], place(dy=a), 8, step)
    arrived(crecv0, 2)
    send_rows(summed(csend0[z * NX + x].astype(F32), crecv0).astype(BF16), dsend0, d0, 3)
    arrived(wo1.at[pl.ds(0, 4), c], 8)
    front, back = pl.ds(0, 64), pl.ds(64, 64)
    send(wo1.at[2, c, front], wo1.at[4, c, front], place(dy=2), 11, step)
    send(wo1.at[6, c, back], wo1.at[4, c, back], place(dy=NY - 2), 11, step)
    send(wo1.at[2, c], wo1.at[3, c], place(dy=1), 11, step)
    send(wo1.at[6, c], wo1.at[5, c], place(dy=NY - 1), 11, step)
    near, far, rest = (wo1.at[pl.ds(first, count), c] for first, count in ((1, 2), (6, 2), (3, 3)))
    given = [send(near, near, partner, 8, swap), send(far, far, partner, 9, swap)]
    arrived(p1recv, 4)
    total_tokens = summed(own_tokens, p1recv)

    arrived(d0.at[pl.ds(0, NX * NZ - 1)], 3)
    half_rows = 2 * NZ
    given.append(send(d0.at[pl.ds(half_rows * other, half_rows)], dpart, partner, 7, swap))
    out = jnp.zeros((NY * ROWS, 512), F32)
    squares_out = cross = squares_step = jnp.zeros((NY * ROWS, 1), F32)
    for half in range(2):
        rows = [
            d0[pl.ds(NZ * (2 * half + part), NZ)].reshape(NZ * ROWS, 128).astype(F32) for part in range(2)
        ]
        rows = jnp.concatenate(rows, axis=1)
        moved = rows * post[half, 0:1, :]
        wide = x0[half].reshape(NY * ROWS, 256).astype(F32)
        squares_out += jnp.sum(rows * rows, axis=1, keepdims=True)
        cross += jnp.sum(wide * moved, axis=1, keepdims=True)
        squares_step += jnp.sum(moved * moved, axis=1, keepdims=True)
        normed = (moved * pre[half, 1:2, :]).astype(BF16)
        out += project(normed, w1.at[half])
    own = jnp.concatenate(
        [out[:, :384], with_columns(out[:, 384:], split_columns([squares_out, cross, squares_step]))], axis=1
    )
    asend1[...] = own.astype(BF16).reshape(NY, ROWS, 512)
    send_along_y(asend1, arecv1, 5)
    own1 = own[:ROWS]
    arrived(rest, 11)
    given.append(send(rest, rest, partner, 10, swap))
    arrived(arecv1, 5)
    total1 = summed(own1, arecv1)
    tail = total1[:, 384:]
    step_scale = lax.rsqrt(stat_of(tail, 0) / D + EPS)
    squares1 = squares0 + step_scale * (2.0 * stat_of(tail, 1) + step_scale * stat_of(tail, 2))
    scale1 = lax.rsqrt(jnp.maximum(squares1, 0.0) / D + EPS)
    mixed, parts = attend(1, (total_tokens[:, :448] + step_scale * total1[:, :448]) * scale1)
    for copy in given:
        copy.wait_recv()
    project_out_all(mixed, csend1)
    send_sums(csend1, crecv1, 6)

    def send_over_chips(source, target, i):
        for k in Y_STEPS + [0]:
            for r in (1, 0):
                if r == 0 and k == 0:
                    continue
                device = {"tp": tp, "dp": lax.rem(y + NY - k, NY) * 2 + (other if r else c)}
                send(source(r * NY + k), target.at[r * NY + k], device, i, step)

    own_scale = jnp.broadcast_to(step_scale, (ROWS, 128))
    ssend[...] = own_scale
    srecv[0] = own_scale
    send_over_chips(lambda slot: ssend, srecv, 9)
    update_state(1, parts)
    arrived(crecv1, 6)
    send_rows(summed(csend1[z * NX + x].astype(F32), crecv1).astype(BF16), dsend1, d1, 7)

    arrived(srecv.at[pl.ds(1, 2 * NY - 1)], 9)
    for r in range(2):
        for k in range(NY):
            a = (NY - k) % NY
            for part in range(2):
                cols = pl.ds(128 * part, 128)
                rows = dpart[NZ * part + a] if r else d0[half_rows * c + NZ * part + a]
                base[r * NY + k, :, cols] = (
                    tok[other if r else c, a, :, cols].astype(F32)
                    + rows.astype(F32) * srecv[r * NY + k] * post[c, 0:1, cols]
                )

    arrived(d1.at[pl.ds(0, NX * NZ - 1)], 7)
    squares_last = jnp.zeros((ROWS, 128), F32)
    for slot in range(NX * NZ):
        rows = d1[slot].astype(F32)
        squares_last += rows * rows
    last_scale = lax.rsqrt(jnp.sum(squares_last, axis=1, keepdims=True) / D + EPS)
    for r in range(2):
        for k in range(NY):
            for part in range(2):
                rows = d1[half_rows * (other if r else c) + NZ * part + k].astype(F32)
                esend[r * NY + k, :, pl.ds(128 * part, 128)] = (rows * last_scale).astype(BF16)
    erecv[0] = esend[0]
    send_over_chips(lambda slot: esend.at[slot], erecv, 10)
    arrived(erecv.at[pl.ds(1, 2 * NY - 1)], 10)
    for r in range(2):
        for k in range(NY):
            value = base[r * NY + k] + erecv[r * NY + k].astype(F32) * post[c, 1:2, :]
            hout[lax.rem(y + k, NY), other if r else c] = value.astype(BF16)
    partial.wait_send()
    for copy in exchanged + given:
        copy.wait_send()
    for ref, i in (
        (arecv0, 0), (arecv1, 5), (p1recv, 4), (b0.at[pl.ds(1, NY - 1)], 1), (wo1.at[pl.ds(0, 4), c], 8), (rest, 11), (crecv0, 2), (crecv1, 6),
        (d0.at[pl.ds(0, NX * NZ - 1)], 3), (d1.at[pl.ds(0, NX * NZ - 1)], 7), (srecv.at[pl.ds(1, 2 * NY - 1)], 9),
        (erecv.at[pl.ds(1, 2 * NY - 1)], 10),
    ):
        sent(ref, i)


def write_out(hidden, state, hidden_out, state_out, done):
    copies = [
        pltpu.make_async_copy(state, state_out, done.at[0]),
        pltpu.make_async_copy(hidden, hidden_out, done.at[1]),
    ]
    for copy in copies:
        copy.start()
    for copy in copies:
        copy.wait()


def local(tokens, recurrent_state, pre_gain, w_query, w_key, w_value, w_gate, w_decay, decay_bias, head_gain, w_out, post_gain):
    vmem = pltpu.VMEM
    dma = pltpu.SemaphoreType.DMA
    blocks = NX * NZ
    hidden, state = pl.pallas_call(
        kernel,
        out_shape=(
            jax.ShapeDtypeStruct((NY, 2, ROWS, 256), BF16),
            jax.ShapeDtypeStruct((2, ROWS, VAL * KEY), F32),
        ),
        in_specs=[pl.BlockSpec(memory_space=pltpu.HBM)] * 12,
        out_specs=[pl.BlockSpec(memory_space=pltpu.VMEM)] * 2,
        scratch_shapes=[
            vmem((2, NY, ROWS, 256), BF16),
            vmem((2, NY, ROWS, 256), BF16),
            vmem((2, ROWS, VAL * KEY), F32),
            vmem((2, 2, 256), F32),
            vmem((2, 2, 256), F32),
            vmem((2, KEY), F32),
            vmem((2, VAL), F32),
            vmem((2, 256, 256), BF16),
            vmem((2, 2, 256, 256), BF16),
            vmem((2, 128, 256), BF16),
            vmem((NY, 2, 128, 256), BF16),
            vmem((NY * ROWS, 512), BF16),
            vmem((NY * ROWS, 512), BF16),
            vmem((NY, ROWS, 512), BF16),
            vmem((NY - 1, ROWS, 512), BF16),
            vmem((NY, ROWS, 512), BF16),
            vmem((NY - 1, ROWS, 512), BF16),
            vmem((NY, ROWS, 512), BF16),
            vmem((NY - 1, ROWS, 512), BF16),
            vmem((NY, ROWS, 128), BF16),
            vmem((blocks, ROWS, 128), BF16),
            vmem((blocks, ROWS, 128), BF16),
            vmem((blocks - 1, ROWS, 128), BF16),
            vmem((blocks - 1, ROWS, 128), BF16),
            vmem((ROWS, 128), BF16),
            vmem((ROWS, 128), BF16),
            vmem((blocks, ROWS, 128), BF16),
            vmem((blocks, ROWS, 128), BF16),
            vmem((2 * NZ, ROWS, 128), BF16),
            vmem((ROWS, 128), F32),
            vmem((2 * NY, ROWS, 128), F32),
            vmem((2 * NY, ROWS, 256), F32),
            vmem((2 * NY, ROWS, 256), BF16),
            vmem((2 * NY, ROWS, 256), BF16),
            dma((18,)),
            dma((11,)),
            dma((11,)),
            dma((12,)),
            dma((12,)),
            pltpu.SemaphoreType.REGULAR,
        ],
        compiler_params=pltpu.CompilerParams(
            collective_id=0, has_side_effects=True, vmem_limit_bytes=32 * 1024 * 1024
        ),
    )(
        *(pltpu.with_memory_space_constraint(v, pltpu.HBM) for v in (
        tokens.reshape(NY, 2, ROWS, 256), recurrent_state, pre_gain, jnp.swapaxes(w_query, 1, 2),
        jnp.swapaxes(w_key, 1, 2), w_value, w_gate, jnp.swapaxes(w_decay, 1, 2),
        decay_bias, head_gain, w_out, post_gain,))
    )
    hidden, state = pl.pallas_call(
        write_out,
        out_shape=(jax.ShapeDtypeStruct(hidden.shape, BF16), jax.ShapeDtypeStruct(state.shape, F32)),
        in_specs=[pl.BlockSpec(memory_space=pl.ANY)] * 2,
        out_specs=[pl.BlockSpec(memory_space=pl.ANY)] * 2,
        scratch_shapes=[dma((2,))],
        compiler_params=pltpu.CompilerParams(vmem_limit_bytes=1024 * 1024),
    )(hidden, state)
    return hidden.reshape(NY * 2 * ROWS, 256), state


def solution(mesh):
    in_specs = (
        P(None, "dp"), P(None, "dp", "tp"), P(None, "dp"), P(None, "dp", "tp"), P(None, "dp", "tp"),
        P(None, "dp", "tp"), P(None, "dp", "tp"), P(None, "dp", "tp"), P(None, "tp"), P(), P(None, "tp", "dp"),
        P(None, "dp"),
    )
    out_specs = (P(None, "dp"), P(None, "dp", "tp"))
    return jax.shard_map(local, mesh=mesh, in_specs=in_specs, out_specs=out_specs, check_vma=False)
```
